32 devices in a mesh: kv: 8 (over z, y), tp: 4 (over x, core).
Axes of the slice: x: 2, y: 2, z: 4, core: 2. Of those that a mesh axis runs over, the one named last changes fastest.
Arguments:
- piece_tokens: bfloat16 [1024, 4096], P('kv'), may hold values from -6 to 6
- decode_tokens: bfloat16 [8, 4096], P('kv'), may hold values from -6 to 6
- norm_gain: bfloat16 [4096], replicated, may hold values from 0.099609375 to 1.8984375
- w_query: bfloat16 [4096, 2048], P(None, 'tp'), may hold values from -0.09375 to 0.09375
- w_key: bfloat16 [4096, 2048], P(None, 'tp'), may hold values from -0.09375 to 0.09375
- w_value: bfloat16 [4096, 2048], P(None, 'tp'), may hold values from -0.09375 to 0.09375
- score_offset: float32 [16], replicated, may hold values from -14 to -3
- context_length: int32 [1], replicated, may hold values from 4096 to 8192
- prompt_keys: bfloat16 [8192, 2048], P('kv', 'tp'), may hold values from -16 to 16, as said below
- prompt_values: bfloat16 [8192, 2048], P('kv', 'tp'), may hold values from -6 to 6
- decode_keys: bfloat16 [8, 1024, 2048], P('kv', None, 'tp'), may hold values from -6 to 6
- decode_values: bfloat16 [8, 1024, 2048], P('kv', None, 'tp'), may hold values from -6 to 6
- decoding_cache_length: int32 [8], P('kv'), may hold values from 1 to 1024, as said below
- out_gain: bfloat16 [2048], replicated, may hold values from 0.099609375 to 1.8984375
- w_out: bfloat16 [2048, 4096], P(None, 'tp'), may hold values from -0.125 to 0.125
Outputs:
- prompt_piece_output: bfloat16 [1024, 4096], P('kv', 'tp')
- decode_out: bfloat16 [8, 4096], P('kv', 'tp')
- piece_keys: bfloat16 [1024, 2048], P('kv', 'tp')
- piece_values: bfloat16 [1024, 2048], P('kv', 'tp')
- decode_new_keys: bfloat16 [8, 2048], P('kv', 'tp')
- decode_new_values: bfloat16 [8, 2048], P('kv', 'tp')
The draws below stay inside these ranges and needn't reach their ends.
Inputs may be any that keep to these rules, and one draw needn't show every extreme that they name: `prompt_keys`: the largest scale of a block of 1024 positions is up to four times the smallest. `decoding_cache_length`: some sequence has exactly 1024 valid positions.
All inputs are finite; a program needn't handle non-finite values.
Results may differ from the reference program's by a relative error of at most 0.008.
The reference program's roundings to bfloat16 on the way count: a program that leaves them out, or rounds other values in their place, can miss the bound.
Values may be sent and summed in bfloat16 or wider, within the bound.
A program may use at most 128 MiB of HBM per device.

```python
import math
import jax
import jax.numpy as jnp
from jax import lax

D = 4096
HEADS = 16
HEAD = 128
PIECE_DEV = 128
CTX_DEV = 1024
DLEN = 1024
PIECE = 1024
CTX = 8192
DEC = 8


def draw_score_offset(key, part):
    key_offset = jax.random.fold_in(key, 3)
    return jax.random.uniform(key_offset, (HEADS,), jnp.float32, -13.0, -3.0)


def draw_prompt_keys(key, part):
    key_scale, key_values = jax.random.split(jax.random.fold_in(key, 5))
    factors = jnp.exp(jax.random.uniform(key_scale, (CTX // CTX_DEV,), jnp.float32, math.log(0.5), math.log(2.0)))
    values = jnp.clip(jax.random.normal(key_values, (CTX, HEADS * HEAD), jnp.float32), -8.0, 8.0)
    places = jnp.arange(CTX, dtype=jnp.int32) // CTX_DEV
    return (values * factors[places][:, None]).astype(jnp.bfloat16)


def draw_decoding_cache_length(key, part):
    key_lengths, key_spot = jax.random.split(jax.random.fold_in(key, 7))
    lengths = jax.random.randint(key_lengths, (DEC,), 1, DLEN + 1, dtype=jnp.int32)
    spot = jax.random.randint(key_spot, (), 0, DEC, dtype=jnp.int32)
    return jnp.where(jnp.arange(DEC, dtype=jnp.int32) == spot, DLEN, lengths).astype(jnp.int32)


def block_scale(key, dims, shards, low, top_value):
    level = 1.0
    for position, parts in shards:
        steps = jax.random.uniform(jax.random.fold_in(jax.random.fold_in(key, 6), position), (parts,), jnp.float32, low / len(shards), top_value / len(shards))
        level = level * jnp.repeat(jnp.exp(steps), dims[position] // parts).reshape((-1,) + (1,) * (len(dims) - 1 - position))
    return level


def scatter_about(own_key, dims, width, reach, shards=(), kind=jnp.bfloat16):
    values = jax.random.normal(own_key, dims, jnp.float32) * width
    if len(shards) > 0:
        values = block_scale(own_key, dims, shards, -0.22, 0.18) * values
    return jnp.clip(values, min=-reach, max=reach).astype(kind)


def setup_inputs(seed: int = 0) -> dict:
    seeds = jax.random.split(jax.random.key(seed), 16)
    piece_tokens = scatter_about(seeds[0], (PIECE, D), 1.0, 6.0, ((0, 8),))
    decode_tokens = scatter_about(seeds[1], (DEC, D), 1.0, 6.0, ((0, 8),))
    norm_gain = jnp.clip(1.0 + 0.18 * jax.random.normal(seeds[2], (D,), jnp.float32), 0.099609375, 1.8984375).astype(jnp.bfloat16)
    w_query = scatter_about(seeds[3], (D, HEADS * HEAD), D ** -0.5, 0.09375, ((1, 4),))
    w_key = scatter_about(seeds[4], (D, HEADS * HEAD), D ** -0.5, 0.09375, ((1, 4),))
    w_value = scatter_about(seeds[5], (D, HEADS * HEAD), D ** -0.5, 0.09375, ((1, 4),))
    score_offset = draw_score_offset(jax.random.fold_in(seeds[15], 71), 0)
    context_length = jax.random.randint(seeds[7], (1,), CTX // 2, CTX + 1).astype(jnp.int32)
    prompt_keys = draw_prompt_keys(jax.random.fold_in(seeds[15], 71), 0)
    prompt_values = scatter_about(seeds[9], (CTX, HEADS * HEAD), 1.0, 6.0, ((0, 8), (1, 4)))
    decode_keys = scatter_about(seeds[10], (DEC, DLEN, HEADS * HEAD), 1.0, 6.0, ((0, 8), (2, 4)))
    decode_values = scatter_about(seeds[11], (DEC, DLEN, HEADS * HEAD), 1.0, 6.0, ((0, 8), (2, 4)))
    decoding_cache_length = draw_decoding_cache_length(jax.random.fold_in(seeds[15], 71), 0)
    out_gain = jnp.clip(1.0 + 0.18 * jax.random.normal(seeds[13], (HEADS * HEAD,), jnp.float32), 0.099609375, 1.8984375).astype(jnp.bfloat16)
    w_out = scatter_about(seeds[14], (HEADS * HEAD, D), (HEADS * HEAD) ** -0.5, 0.125, ((1, 4),))
    return {"piece_tokens": piece_tokens, "decode_tokens": decode_tokens, "norm_gain": norm_gain, "w_query": w_query, "w_key": w_key, "w_value": w_value, "score_offset": score_offset, "context_length": context_length, "prompt_keys": prompt_keys, "prompt_values": prompt_values, "decode_keys": decode_keys, "decode_values": decode_values, "decoding_cache_length": decoding_cache_length, "out_gain": out_gain, "w_out": w_out}


EPS = 1e-06

def rms_scaled(rows, gain):
    values = rows.astype(jnp.float32)
    inverse = lax.rsqrt(lax.optimization_barrier(jnp.mean(values * values, axis=-1, keepdims=True)) + EPS)
    return values * inverse * gain.astype(jnp.float32)

def block_terms(scores, visible):
    keep = jnp.where(visible, jax.nn.log_sigmoid(-scores), 0.0)
    after = lax.cumsum(keep, axis=scores.ndim - 1, reverse=True) - keep
    weight = jnp.where(visible, jnp.exp(jax.nn.log_sigmoid(scores) + after), 0.0)
    return (weight.astype(jnp.bfloat16), lax.optimization_barrier(jnp.sum(keep, axis=-1)))

def reference(piece_tokens, decode_tokens, norm_gain, w_query, w_key, w_value, score_offset, context_length, prompt_keys, prompt_values, decode_keys, decode_values, decoding_cache_length, out_gain, w_out):
    all_rows = jnp.concatenate([piece_tokens, decode_tokens], axis=0)
    normed_in = rms_scaled(all_rows, norm_gain).astype(jnp.bfloat16)
    queries = jnp.dot(normed_in, w_query, preferred_element_type=jnp.float32).astype(jnp.bfloat16)
    new_keys = jnp.dot(normed_in, w_key, preferred_element_type=jnp.float32).astype(jnp.bfloat16)
    new_values = jnp.dot(normed_in, w_value, preferred_element_type=jnp.float32).astype(jnp.bfloat16)
    score_scale = HEAD ** (-0.5)

    def by_head(matrix, span):
        return matrix.reshape(-1, HEADS, HEAD).transpose(1, 0, 2).reshape(HEADS, -1, span, HEAD)
    piece_queries = queries[:PIECE].reshape(PIECE, HEADS, HEAD).transpose(1, 0, 2)
    cache_k = by_head(prompt_keys, CTX_DEV)
    cached_value_rows = by_head(prompt_values, CTX_DEV)
    piece_k = by_head(new_keys[:PIECE], PIECE_DEV)
    piece_v = by_head(new_values[:PIECE], PIECE_DEV)
    cache_places = jnp.arange(CTX, dtype=jnp.int32).reshape(-1, CTX_DEV)
    valid_mask = cache_places < context_length[0]
    piece_places = jnp.arange(PIECE, dtype=jnp.int32).reshape(-1, PIECE_DEV)

    def per_head(inputs_tuple):
        head_q, head_ck, head_cached_values, head_pk, head_prompt_values, head_offset = inputs_tuple

        def per_block(block_index):
            start = block_index * PIECE_DEV
            query_rows = lax.dynamic_slice_in_dim(head_q, start, PIECE_DEV, 0)
            query_places = start + jnp.arange(PIECE_DEV, dtype=jnp.int32)
            cache_scores = jnp.dot(query_rows, head_ck.reshape(-1, HEAD).T, preferred_element_type=jnp.float32).reshape(PIECE_DEV, -1, CTX_DEV)
            cache_scores = cache_scores * score_scale + head_offset
            cached_weight_rows, cache_total = block_terms(cache_scores, valid_mask[None])
            cached_output = jnp.einsum('vef,efw->vew', cached_weight_rows.astype(jnp.float32), head_cached_values.astype(jnp.float32))
            piece_scores = jnp.dot(query_rows, head_pk.reshape(-1, HEAD).T, preferred_element_type=jnp.float32).reshape(PIECE_DEV, -1, PIECE_DEV)
            piece_scores = piece_scores * score_scale + head_offset
            seen = piece_places[None] < query_places[:, None, None]
            prompt_piece_weight, piece_total = block_terms(piece_scores, seen)
            prompt_piece_output = jnp.einsum('vef,efw->vew', prompt_piece_weight.astype(jnp.float32), head_prompt_values.astype(jnp.float32))
            later_cache = lax.cumsum(cache_total, axis=1, reverse=True) - cache_total
            later_piece = lax.cumsum(piece_total, axis=1, reverse=True) - piece_total
            piece_sum = lax.optimization_barrier(jnp.sum(piece_total, axis=1, keepdims=True))
            mixed = lax.optimization_barrier(jnp.sum(cached_output * jnp.exp(later_cache + piece_sum)[:, :, None], axis=1))
            mixed = mixed + lax.optimization_barrier(jnp.sum(prompt_piece_output * jnp.exp(later_piece)[:, :, None], axis=1))
            return mixed.astype(jnp.bfloat16)
        return lax.map(per_block, jnp.arange(PIECE // PIECE_DEV, dtype=jnp.int32)).reshape(PIECE, HEAD)
    piece_heads = lax.map(per_head, (piece_queries, cache_k, cached_value_rows, piece_k, piece_v, score_offset))
    piece_attention = piece_heads.transpose(1, 0, 2).reshape(PIECE, HEADS * HEAD)
    decode_queries = queries[PIECE:].reshape(DEC, HEADS, HEAD)

    def per_sequence(inputs_tuple):
        seq_q, seq_k, seq_v, seq_length = inputs_tuple
        keys_heads = seq_k.reshape(DLEN, HEADS, HEAD).astype(jnp.float32)
        values_heads = seq_v.reshape(DLEN, HEADS, HEAD).astype(jnp.float32)
        scores = jnp.einsum('hd,khd->hk', seq_q.astype(jnp.float32), keys_heads) * score_scale
        scores = scores + score_offset[:, None]
        seen = jnp.arange(DLEN, dtype=jnp.int32)[None, :] < seq_length
        weight, unused = block_terms(scores, seen)
        result = jnp.einsum('hk,khd->hd', weight.astype(jnp.float32), values_heads)
        return result.astype(jnp.bfloat16).reshape(HEADS * HEAD)
    decode_attention = lax.map(per_sequence, (decode_queries, decode_keys, decode_values, decoding_cache_length))
    attention = jnp.concatenate([piece_attention, decode_attention], axis=0)
    normed_out = rms_scaled(attention, out_gain).astype(jnp.bfloat16)
    outputs = jnp.dot(normed_out, w_out, preferred_element_type=jnp.float32).astype(jnp.bfloat16)
    return (outputs[:PIECE], outputs[PIECE:], new_keys[:PIECE], new_values[:PIECE], new_keys[PIECE:], new_values[PIECE:])
```

```python
import functools
import math

import jax
import jax.numpy as jnp
from jax import lax
from jax.experimental import pallas as pl
from jax.experimental.pallas import tpu as pltpu
from jax.sharding import PartitionSpec as P

HEAD = 128
EPS = 1e-06
HIDDEN = -1e30
LOG2E = 1.4426950408889634
MESH = pl.DeviceIdType.MESH


def rms_scaled(rows, gain):
    values = rows.astype(jnp.float32)
    inverse = lax.rsqrt(jnp.mean(values * values, axis=-1, keepdims=True) + EPS)
    return values * inverse * gain.astype(jnp.float32)


def suffix_matrix(size):
    row = lax.broadcasted_iota(jnp.int32, (size, size), 0)
    column = lax.broadcasted_iota(jnp.int32, (size, size), 1)
    return jnp.where(row >= column, 1.0, 0.0).astype(jnp.bfloat16)


def spread_matrix(size):
    run = size // 8
    row = lax.broadcasted_iota(jnp.int32, (size, size), 0)
    column = lax.broadcasted_iota(jnp.int32, (size, size), 1)
    hit = (row // 8 == column % run) & (row % 8 == column // run)
    return jnp.where(hit, 1.0, 0.0).astype(jnp.bfloat16)


def dot_t(a, b):
    return lax.dot_general(a, b, (((1,), (1,)), ((), ())), preferred_element_type=jnp.float32)


def dot(a, b):
    return jnp.dot(a, b, preferred_element_type=jnp.float32)


def suffix_keep(z, suffix):
    keep = -(jnp.maximum(z, 0.0) + jnp.log(1.0 + jnp.exp(-jnp.abs(z))))
    high = keep.astype(jnp.bfloat16)
    low = (keep - high.astype(jnp.float32)).astype(jnp.bfloat16)
    return dot(high, suffix) + dot(low, suffix)


def cached_terms(query, key_of, value_of, bias_of, total_keys, chunk, suffix, scale):
    later = None
    out = None
    for start in reversed(range(0, total_keys, chunk)):
        z = dot_t(query, key_of(start)) * scale + bias_of(start)
        inner = suffix_keep(z, suffix)
        exponent = z + inner if later is None else z + inner + later
        weight = jnp.exp(exponent).astype(jnp.bfloat16)
        part = dot(weight, value_of(start))
        out = part if out is None else out + part
        later = inner[:, 0:1] if later is None else later + inner[:, 0:1]
    return out, later


def grid_of(n):
    columns = max(d for d in range(1, math.isqrt(n) + 1) if n % d == 0)
    return n // columns, columns


def later_sublanes(runs):
    place = lax.broadcasted_iota(jnp.int32, runs.shape, 0)

    def up(x, k):
        return jnp.where(place < 8 - k, pltpu.roll(x, 8 - k, 0), 1.0)

    x = up(runs, 1)
    x = x * up(x, 1)
    x = x * up(x, 2)
    return x * up(x, 4)


def break_sticks(score, store, steps, groups):
    left = [jnp.ones((8, 128), jnp.float32) for _ in range(groups)]
    for v in reversed(range(steps)):
        for g in range(groups):
            e = jnp.exp2(jnp.minimum(score(v, g), 126.0))
            left[g] = left[g] * (1.0 / (1.0 + e))
            store(v, g, e * left[g])
    return left


def attention_kernel(
    nz, ny, tp, heads, q_ref, k_ref, v_ref, dq_ref, ck_ref, cv_ref, dk_ref, dv_ref, gain_ref, off_ref,
    ctx_ref, len_ref, out_ref,
    qg, kp, vt, tab, zbuf, own, obuf, tbuf, oy, ty, mix, zs, zt, zr, ztr, zmix,
    kvb, kvg, qp, pz, pacc, plat, ps, pt, pr, ptr, att, attg,
    q_ys, q_zs, q_fs, q_rs, kv_zs, kv_ys, kv_fs, kv_rs, oy_s, oy_r, ty_s, ty_r, oz_s, oz_r, tz_s, tz_r,
    p_s, p_r, pt_s, pt_r, a_s, a_r,
):
    n = nz * ny
    me = lax.axis_index("kv")
    mine = lax.axis_index("tp")
    z = me // ny
    y = lax.rem(me, ny)
    rows = q_ref.shape[0]
    width = heads * HEAD
    cache_rows = ck_ref.shape[0]
    seqs, slots = dk_ref.shape[0], dk_ref.shape[1]
    scale = HEAD ** (-0.5)
    scale2 = scale * LOG2E
    halves = nz // heads
    my_head = lax.rem(z, heads)
    my_part = z // heads
    bits = nz.bit_length() - 1
    paired = nz == 1 << bits

    def turned(s):
        total = 0
        for b in range(bits):
            total += lax.rem(lax.rem(z // (1 << b), 2) + lax.rem(s // (1 << b), 2), 2) * (1 << b)
        return total

    def source(s):
        return turned(s) if paired else lax.rem(z + s, nz)

    def target(s):
        return turned(s) if paired else lax.rem(z + nz - s, nz)

    def other(k):
        return lax.rem(y + k, ny)

    def head_cols(h):
        return pl.ds(h * HEAD, HEAD)

    barrier = pltpu.get_barrier_semaphore()
    for s in range(1, n):
        pl.semaphore_signal(barrier, inc=1, device_id={"kv": lax.rem(me + s, n)}, device_id_type=MESH)
    for s in range(1, tp):
        pl.semaphore_signal(barrier, inc=1, device_id={"tp": lax.rem(mine + s, tp)}, device_id_type=MESH)
    pl.semaphore_wait(barrier, n - 1 + tp - 1)

    def remote(src, dst, ss, rs, peer, axis="kv"):
        return pltpu.make_async_remote_copy(
            src_ref=src, dst_ref=dst, send_sem=ss, recv_sem=rs,
            device_id={axis: peer}, device_id_type=MESH,
        )

    def q_plane(s):
        return remote(q_ref, qg.at[me], q_zs.at[s], q_rs.at[me], target(s) * ny + y)

    def q_column(k):
        return remote(q_ref, qg.at[me], q_ys.at[k], q_rs.at[me], z * ny + other(k))

    def q_block(c, s, k):
        return remote(qg.at[c], qg.at[c], q_fs.at[s, k], q_rs.at[c], z * ny + other(k))

    for s in range(1, nz):
        q_plane(s).start()
    for k in range(1, ny):
        q_column(k).start()
    qg[me] = q_ref[...]

    short = spread_matrix(rows)
    for h in range(heads):
        kvb[h, 0:rows, :] = dot(short, k_ref[:, head_cols(h)]).astype(jnp.bfloat16)
        kvb[h, rows : 2 * rows, :] = jnp.transpose(dot(short, v_ref[:, head_cols(h)])).astype(jnp.bfloat16)

    def kv_plane(t):
        return remote(kvb.at[t % heads], kvg.at[me], kv_zs.at[t], kv_rs.at[me], t * ny + y)

    def kv_column(k):
        return remote(kvb.at[my_head], kvg.at[me], kv_ys.at[k], kv_rs.at[me], z * ny + other(k))

    def kv_block(c, s, k):
        return remote(kvg.at[c], kvg.at[c], kv_fs.at[s, k], kv_rs.at[c], z * ny + other(k))

    for t in range(nz):
        pl.when(z != t)(lambda t=t: kv_plane(t).start())
    for k in range(1, ny):
        kv_column(k).start()
    kvg[me] = kvb[my_head]

    run = cache_rows // 8
    tiles = run // 32
    wide = spread_matrix(256)
    for t in range(tiles):
        def strip(ref):
            return jnp.concatenate([ref[pl.ds(s * run + t * 32, 32), :] for s in range(8)], axis=0)
        keys = dot(wide, strip(ck_ref)).astype(jnp.bfloat16)
        values = dot(wide, strip(cv_ref))
        for h in range(heads):
            kp[h, t * 256 : t * 256 + 256, :] = keys[:, h * HEAD : h * HEAD + HEAD]
            vt[h, :, t * 256 : t * 256 + 256] = jnp.transpose(
                values[:, h * HEAD : h * HEAD + HEAD]
            ).astype(jnp.bfloat16)
    row = lax.broadcasted_iota(jnp.int32, (cache_rows, 128), 0)
    valid = me * cache_rows + lax.rem(row, 8) * run + row // 8 < ctx_ref[0]
    for h in range(heads):
        tab[h] = jnp.where(valid, off_ref[mine * heads + h] * LOG2E, HIDDEN)

    chunk = 256 if slots % 256 == 0 else 128
    suffix = suffix_matrix(chunk)
    hrow = lax.broadcasted_iota(jnp.int32, (8, width), 0)
    hcol = lax.broadcasted_iota(jnp.int32, (8, width), 1) // HEAD
    own_head = hrow == hcol
    head_row = lax.broadcasted_iota(jnp.int32, (8, chunk), 0)
    spot = lax.broadcasted_iota(jnp.int32, (8, chunk), 1)
    offsets = jnp.zeros((8, chunk), jnp.float32)
    for h in range(heads):
        offsets = jnp.where(head_row == h, off_ref[mine * heads + h], offsets)
    dec_rows = jnp.zeros((16, width), jnp.float32)
    for b in range(seqs):
        query = jnp.where(own_head, dq_ref[b : b + 1, :].astype(jnp.float32), 0.0).astype(jnp.bfloat16)
        out, unused = cached_terms(
            query,
            lambda start: dk_ref[b, pl.ds(start, chunk), :],
            lambda start: dv_ref[b, pl.ds(start, chunk), :],
            lambda start: jnp.where(spot + start < len_ref[b], offsets, HIDDEN),
            slots, chunk, suffix, scale,
        )
        line = jnp.sum(jnp.where(own_head, out, 0.0), axis=0, keepdims=True)
        place = lax.broadcasted_iota(jnp.int32, (16, width), 0)
        dec_rows = jnp.where(place == b, line, dec_rows)
    att[pl.ds(rows, 16), :] = dec_rows.astype(att.dtype)

    def forward(s):
        c = source(s) * ny + y
        q_block(c, s, 0).wait_recv()
        kv_block(c, s, 0).wait_recv()
        for k in range(1, ny):
            q_block(c, s, k).start()
            kv_block(c, s, k).start()

    def piece_out(j):
        return remote(ps.at[j], pr.at[my_head], p_s.at[j], p_r.at[my_head], (my_part + halves * j) * ny + y)

    def piece_total(j):
        return remote(pt.at[j], ptr.at[my_head], pt_s.at[j], pt_r.at[my_head], (my_part + halves * j) * ny + y)

    def pieces():
        for k in range(1, ny):
            for u in range(nz):
                kv_block(u * ny + other(k), 0, 0).wait_recv()
        cols = pl.ds(pl.multiple_of(my_head * HEAD, HEAD), HEAD)
        for j in range(heads):
            qp[j * rows : j * rows + rows, :] = qg[(my_part + halves * j) * ny + y, :, cols]
        pacc[...] = jnp.zeros_like(pacc)
        plat[...] = jnp.ones_like(plat)
        lane = lax.broadcasted_iota(jnp.int32, (8, 128), 1)
        first = lax.broadcasted_iota(jnp.int32, (8, 128), 0) * (rows // 8)
        off = off_ref[mine * heads + my_head] * LOG2E

        def block(i, carry):
            c = n - 1 - i
            pz[...] = dot_t(kvg[c, 0:rows, :], qp[...])

            def score(v, g):
                seen = c * rows + first + v < ((my_part + halves * g) * ny + y) * rows + lane
                return jnp.where(seen, pz[v * 8 : v * 8 + 8, g * 128 : g * 128 + 128] * scale2 + off, HIDDEN)

            def store(v, g, w):
                pz[v * 8 : v * 8 + 8, g * 128 : g * 128 + 128] = w

            left = break_sticks(score, store, rows // 8, heads)
            factors = [later_sublanes(x) for x in left]
            factor = jnp.concatenate(factors, axis=1)
            w = pz[...].reshape(rows // 8, 8, heads * rows) * factor[None]
            w = w.reshape(rows, heads * rows).astype(jnp.bfloat16)
            pacc[...] += dot(kvg[c, rows : 2 * rows, :], w) * plat[0:1, :]
            whole = (factor * jnp.concatenate(left, axis=1))[0:1, :]
            plat[...] = plat[...] * whole
            return carry

        lax.fori_loop(0, n, block, 0)
        for j in range(heads):
            owner = my_part + halves * j
            ps[j] = pacc[:, j * rows : j * rows + rows].astype(jnp.bfloat16)
            pt[j] = plat[:, j * rows : j * rows + rows]

            @pl.when(owner != z)
            def _():
                piece_out(j).start()
                piece_total(j).start()

            @pl.when(owner == z)
            def _():
                pr[my_head] = ps[j]
                ptr[my_head] = pt[j]

    def o_column(u, s, k):
        return remote(obuf.at[u, other(k)], oy.at[u, y], oy_s.at[s, k], oy_r.at[u, y], z * ny + other(k))

    def t_column(u, s, k):
        return remote(tbuf.at[u, other(k)], ty.at[u, y], ty_s.at[s, k], ty_r.at[u, y], z * ny + other(k))

    def o_from(u, c):
        return remote(obuf.at[u, c], oy.at[u, c], oy_s.at[0, 0], oy_r.at[u, c], z * ny + other(1))

    def t_from(u, c):
        return remote(tbuf.at[u, c], ty.at[u, c], ty_s.at[0, 0], ty_r.at[u, c], z * ny + other(1))

    def compute(u):
        totals = [jnp.ones((8, 128), jnp.float32) for _ in range(ny)]
        place = lax.broadcasted_iota(jnp.int32, (8, 128), 0)
        for h in range(heads):
            q = qg[pl.ds(u * ny, ny), :, head_cols(h)].reshape(ny * rows, HEAD)
            zbuf[h] = dot_t(kp[h], q)

            def score(v, g):
                at = slice(v * 8, v * 8 + 8)
                return zbuf[h, at, g * 128 : g * 128 + 128] * scale2 + tab[h, at, :]

            def store(v, g, w):
                zbuf[h, v * 8 : v * 8 + 8, g * 128 : g * 128 + 128] = w

            left = break_sticks(score, store, run, ny)
            factors = [later_sublanes(x) for x in left]
            factor = jnp.concatenate(factors, axis=1)
            w = zbuf[h].reshape(run, 8, ny * rows) * factor[None]
            out = dot(vt[h], w.reshape(cache_rows, ny * rows).astype(jnp.bfloat16))
            for g in range(ny):
                part = out[:, g * rows : g * rows + rows]
                own[u, g, head_cols(h), :] = part
                obuf[u, g, head_cols(h), :] = part.astype(jnp.bfloat16)
                totals[g] = jnp.where(place == h, (factors[g] * left[g])[0:1, :], totals[g])
        for g in range(ny):
            tbuf[u, g] = totals[g]
        ty[u, y] = tbuf[u, y]

    def o_plane(u, s):
        return remote(zs.at[u], zr.at[z], oz_s.at[s], oz_r.at[z], u * ny + y)

    def t_plane(u, s):
        return remote(zt.at[u], ztr.at[z], tz_s.at[s], tz_r.at[z], u * ny + y)

    def combine(s):
        u = source(s)
        mix[y] = own[u, y]
        for k in range(1, ny):
            o_from(u, other(k)).wait_recv()
            t_from(u, other(k)).wait_recv()
            mix[other(k)] = oy[u, other(k)].astype(jnp.float32)
        later = jnp.ones((8, 128), jnp.float32)
        factors = []
        for c in reversed(range(ny)):
            factors.append(later)
            later = later * ty[u, c]
        for h in range(heads):
            total = jnp.zeros((HEAD, rows), jnp.float32)
            for c in range(ny):
                total += mix[c, head_cols(h), :] * factors[ny - 1 - c][h : h + 1, :]
            zs[u, head_cols(h), :] = total.astype(jnp.bfloat16)

            @pl.when(u == z)
            def _():
                zmix[z, head_cols(h), :] = total

        zt[u] = later

        @pl.when(u == z)
        def _():
            ztr[z] = later

        @pl.when(u != z)
        def _():
            o_plane(u, s).start()
            t_plane(u, s).start()

    def step(s, carry):
        u = source(s)
        pl.when(s + 1 < nz)(lambda: forward(s + 1))
        for k in range(1, ny):
            q_block(u * ny + other(k), 0, 0).wait_recv()
        pl.when(s == nz - 1)(pieces)
        compute(u)
        for k in range(1, ny):
            o_column(u, s, k).start()
            t_column(u, s, k).start()
        pl.when(s > 0)(lambda: combine(s - 1))
        return carry

    lax.fori_loop(0, nz, step, 0)
    combine(nz - 1)

    for h in range(heads):
        plane = lax.rem(z, halves) * heads + h

        @pl.when(plane != z)
        def _():
            remote(ps.at[0], pr.at[h], p_s.at[0], p_r.at[h], plane * ny + y).wait_recv()
            remote(pt.at[0], ptr.at[h], pt_s.at[0], pt_r.at[h], plane * ny + y).wait_recv()

    for s in range(1, nz):
        u = source(s)
        remote(zs.at[u], zr.at[u], oz_s.at[s], oz_r.at[u], u * ny + y).wait_recv()
        remote(zt.at[u], ztr.at[u], tz_s.at[s], tz_r.at[u], u * ny + y).wait_recv()
        zmix[u] = zr[u].astype(jnp.float32)

    later = jnp.ones((8, 128), jnp.float32)
    factors = []
    for c in reversed(range(nz)):
        factors.append(later)
        later = later * ztr[c]
    for h in range(heads):
        total = jnp.zeros((HEAD, rows), jnp.float32)
        for c in range(nz):
            total += zmix[c, head_cols(h), :] * factors[nz - 1 - c][h : h + 1, :]
        total = total * ptr[h, 0:1, :] + pr[h].astype(jnp.float32)
        att[pl.ds(0, rows), head_cols(h)] = jnp.transpose(total).astype(att.dtype)

    for s in range(1, tp):
        peer = lax.rem(mine + s, tp)
        remote(att, attg.at[mine], a_s.at[s], a_r.at[mine], peer, "tp").start()
    attg[mine] = att[...]

    for s in range(1, nz):
        q_plane(s).wait_send()
        u = source(s)
        c = u * ny + y
        o_plane(u, s).wait_send()
        t_plane(u, s).wait_send()
        for k in range(1, ny):
            q_block(c, s, k).wait_send()
            kv_block(c, s, k).wait_send()
    for t in range(nz):
        pl.when(z != t)(lambda t=t: kv_plane(t).wait_send())
    for k in range(1, ny):
        q_column(k).wait_send()
        kv_column(k).wait_send()
        for s in range(nz):
            o_column(source(s), s, k).wait_send()
            t_column(source(s), s, k).wait_send()
    for j in range(heads):

        @pl.when(my_part + halves * j != z)
        def _():
            piece_out(j).wait_send()
            piece_total(j).wait_send()

    for s in range(1, tp):
        peer = lax.rem(mine + s, tp)
        remote(att, attg.at[peer], a_s.at[s], a_r.at[peer], peer, "tp").wait()
    square = jnp.zeros((att.shape[0], 1), jnp.float32)
    for t in range(tp):
        values = attg[t].astype(jnp.float32)
        square += jnp.sum(values * values, axis=-1, keepdims=True)
    inverse = lax.rsqrt(square / (tp * width) + EPS)
    for t in range(tp):
        cols = pl.ds(t * width, width)
        gain = gain_ref[0:1, cols].astype(jnp.float32)
        out_ref[:, cols] = (attg[t].astype(jnp.float32) * inverse * gain).astype(out_ref.dtype)


def attend(
    nz, ny, tp, queries, keys, values, decode_queries, prompt_keys, prompt_values, decode_keys, decode_values,
    out_gain, score_offset, context_length, decoding_cache_length,
):
    n = nz * ny
    rows, width = queries.shape
    heads = width // HEAD
    assert nz % heads == 0
    cache_rows = prompt_keys.shape[0]
    vmem = pl.BlockSpec(memory_space=pltpu.VMEM)
    smem = pl.BlockSpec(memory_space=pltpu.SMEM)
    dma = pltpu.SemaphoreType.DMA

    def half(*shape):
        return pltpu.VMEM(shape, jnp.bfloat16)

    def full(*shape):
        return pltpu.VMEM(shape, jnp.float32)

    return pl.pallas_call(
        functools.partial(attention_kernel, nz, ny, tp, heads),
        out_shape=jax.ShapeDtypeStruct((rows + 16, tp * width), jnp.bfloat16),
        in_specs=[vmem] * 9 + [smem] * 3,
        out_specs=vmem,
        scratch_shapes=[
            half(n, rows, width), half(heads, cache_rows, HEAD), half(heads, HEAD, cache_rows),
            full(heads, cache_rows, 128), full(heads, cache_rows, ny * rows),
            full(nz, ny, width, rows), half(nz, ny, width, rows), full(nz, ny, 8, 128),
            half(nz, ny, width, rows), full(nz, ny, 8, 128), full(ny, width, rows),
            half(nz, width, rows), full(nz, 8, 128), half(nz, width, rows), full(nz, 8, 128),
            full(nz, width, rows),
            half(heads, 2 * rows, HEAD), half(n, 2 * rows, HEAD), half(heads * rows, HEAD),
            full(rows, heads * rows), full(HEAD, heads * rows), full(8, heads * rows),
            half(heads, HEAD, rows), full(heads, 8, 128), half(heads, HEAD, rows), full(heads, 8, 128),
            half(rows + 16, width), half(tp, rows + 16, width),
            dma((ny,)), dma((nz,)), dma((nz, ny)), dma((n,)),
            dma((nz,)), dma((ny,)), dma((nz, ny)), dma((n,)),
            dma((nz, ny)), dma((nz, ny)), dma((nz, ny)), dma((nz, ny)),
            dma((nz,)), dma((nz,)), dma((nz,)), dma((nz,)),
            dma((heads,)), dma((heads,)), dma((heads,)), dma((heads,)),
            dma((tp,)), dma((tp,)),
        ],
        compiler_params=pltpu.CompilerParams(
            collective_id=0, has_side_effects=True, vmem_limit_bytes=56 * 1024 * 1024
        ),
        name="attend",
    )(
        queries, keys, values, decode_queries, prompt_keys, prompt_values, decode_keys, decode_values,
        out_gain[None, :], score_offset, context_length, decoding_cache_length,
    )


def body(
    piece_tokens, decode_tokens, norm_gain, w_query, w_key, w_value, score_offset, context_length,
    prompt_keys, prompt_values, decode_keys, decode_values, decoding_cache_length, out_gain, w_out,
):
    n, tp = lax.axis_size("kv"), lax.axis_size("tp")
    nz, ny = grid_of(n)
    rows = piece_tokens.shape[0]
    seqs = decode_keys.shape[0]
    all_rows = jnp.concatenate([piece_tokens, decode_tokens], axis=0)
    normed_in = rms_scaled(all_rows, norm_gain).astype(jnp.bfloat16)
    queries = jnp.dot(normed_in, w_query, preferred_element_type=jnp.float32).astype(jnp.bfloat16)
    new_keys = jnp.dot(normed_in, w_key, preferred_element_type=jnp.float32).astype(jnp.bfloat16)
    new_values = jnp.dot(normed_in, w_value, preferred_element_type=jnp.float32).astype(
        jnp.bfloat16
    )
    normed_out = attend(
        nz, ny, tp, queries[:rows], new_keys[:rows], new_values[:rows], queries[rows:], prompt_keys,
        prompt_values, decode_keys, decode_values, out_gain, score_offset, context_length,
        decoding_cache_length,
    )
    outputs = jnp.dot(normed_out, w_out, preferred_element_type=jnp.float32).astype(jnp.bfloat16)
    return (
        outputs[:rows],
        outputs[rows : rows + seqs],
        new_keys[:rows],
        new_values[:rows],
        new_keys[rows:],
        new_values[rows:],
    )


def solution(mesh):
    in_specs = (
        P("kv", None),
        P("kv", None),
        P(),
        P(None, "tp"),
        P(None, "tp"),
        P(None, "tp"),
        P(),
        P(),
        P("kv", "tp"),
        P("kv", "tp"),
        P("kv", None, "tp"),
        P("kv", None, "tp"),
        P("kv"),
        P(),
        P(None, "tp"),
    )
    out_specs = (
        P("kv", "tp"),
        P("kv", "tp"),
        P("kv", "tp"),
        P("kv", "tp"),
        P("kv", "tp"),
        P("kv", "tp"),
    )
    return jax.shard_map(body, mesh=mesh, in_specs=in_specs, out_specs=out_specs, check_vma=False)
```

```python
import functools
import math

import jax
import jax.numpy as jnp
from jax import lax
from jax.experimental import pallas as pl
from jax.experimental.pallas import tpu as pltpu
from jax.sharding import PartitionSpec as P

HEAD = 128
EPS = 1e-06
HIDDEN = -1e30
LOG2E = 1.4426950408889634
MESH = pl.DeviceIdType.MESH


def rms_scaled(rows, gain):
    values = rows.astype(jnp.float32)
    inverse = lax.rsqrt(jnp.mean(values * values, axis=-1, keepdims=True) + EPS)
    return values * inverse * gain


def suffix_matrix(size):
    row = lax.broadcasted_iota(jnp.int32, (size, size), 0)
    column = lax.broadcasted_iota(jnp.int32, (size, size), 1)
    return jnp.where(row >= column, 1.0, 0.0).astype(jnp.bfloat16)


def spread_matrix(size):
    run = size // 8
    row = lax.broadcasted_iota(jnp.int32, (size, size), 0)
    column = lax.broadcasted_iota(jnp.int32, (size, size), 1)
    hit = (row // 8 == column % run) & (row % 8 == column // run)
    return jnp.where(hit, 1.0, 0.0).astype(jnp.bfloat16)


def dot_t(a, b):
    return lax.dot_general(a, b, (((1,), (1,)), ((), ())), preferred_element_type=jnp.float32)


def dot(a, b):
    return jnp.dot(a, b, preferred_element_type=jnp.float32)


def suffix_keep(z, suffix):
    keep = -(jnp.maximum(z, 0.0) + jnp.log(1.0 + jnp.exp(-jnp.abs(z))))
    high = keep.astype(jnp.bfloat16)
    low = (keep - high.astype(jnp.float32)).astype(jnp.bfloat16)
    return dot(high, suffix) + dot(low, suffix)


def cached_terms(query, key_of, value_of, bias_of, total_keys, chunk, suffix, scale):
    later = None
    out = None
    for start in reversed(range(0, total_keys, chunk)):
        z = dot_t(query, key_of(start)) * scale + bias_of(start)
        inner = suffix_keep(z, suffix)
        exponent = z + inner if later is None else z + inner + later
        weight = jnp.exp(exponent).astype(jnp.bfloat16)
        part = dot(weight, value_of(start))
        out = part if out is None else out + part
        later = inner[:, 0:1] if later is None else later + inner[:, 0:1]
    return out, later


def grid_of(n):
    columns = max(d for d in range(1, math.isqrt(n) + 1) if n % d == 0)
    return n // columns, columns


def later_sublanes(runs):
    place = lax.broadcasted_iota(jnp.int32, runs.shape, 0)

    def up(x, k):
        return jnp.where(place < 8 - k, pltpu.roll(x, 8 - k, 0), 1.0)

    x = up(runs, 1)
    x = x * up(x, 1)
    x = x * up(x, 2)
    return x * up(x, 4)


def break_sticks(score, store, steps, groups):
    left = [jnp.ones((8, 128), jnp.float32) for _ in range(groups)]
    for v in reversed(range(steps)):
        for g in range(groups):
            e = jnp.exp2(jnp.minimum(score(v, g), 126.0))
            left[g] = left[g] * (1.0 / (1.0 + e))
            store(v, g, e * left[g])
    return left


def attention_kernel(
    nz, ny, tp, heads, x_hbm, d_hbm, wq_hbm, wk_hbm, wv_hbm, ck_hbm, cv_hbm, dk_hbm, dv_hbm, wo_hbm,
    in_gain_ref, gain_ref, off_ref, ctx_ref, len_ref, out_ref, dec_ref, k_out, v_out, dec_k_ref, dec_v_ref,
    x_ref, d_ref, wq_ref, wk_ref, wv_ref, ck_ref, cv_ref, dk_ref, dv_ref, wo_ref,
    xs, q_ref, k_ref, v_ref, dq_ref, normed,
    qg, kp, vt, tab, zbuf, own, obuf, tbuf, oy, ty, mix, zs, zt, zr, ztr, zmix,
    kvb, kvg, qp, pz, pacc, plat, ps, pt, pr, ptr, att, attg,
    q_ys, q_zs, q_fs, q_rs, kv_zs, kv_ys, kv_fs, kv_rs, oy_s, oy_r, ty_s, ty_r, oz_s, oz_r, tz_s, tz_r,
    p_s, p_r, pt_s, pt_r, a_s, a_r, b_s, load_s, w_s, keep_s,
):
    n = nz * ny
    me = lax.axis_index("kv")
    mine = lax.axis_index("tp")
    z = me // ny
    y = lax.rem(me, ny)
    rows = x_hbm.shape[0]
    width = heads * HEAD
    cache_rows = ck_ref.shape[0]
    seqs, slots = dk_hbm.shape[0], dk_hbm.shape[1]
    scale = HEAD ** (-0.5)
    scale2 = scale * LOG2E
    halves = nz // heads
    my_head = lax.rem(z, heads)
    my_part = z // heads
    bits = nz.bit_length() - 1
    paired = nz == 1 << bits

    def turned(s):
        total = 0
        for b in range(bits):
            total += lax.rem(lax.rem(z // (1 << b), 2) + lax.rem(s // (1 << b), 2), 2) * (1 << b)
        return total

    def source(s):
        return turned(s) if paired else lax.rem(z + s, nz)

    def target(s):
        return turned(s) if paired else lax.rem(z + nz - s, nz)

    def other(k):
        return lax.rem(y + k, ny)

    def head_cols(h):
        return pl.ds(h * HEAD, HEAD)

    feed = pltpu.make_async_copy(x_hbm, x_ref, load_s.at[4])
    feed.start()
    feed_one = pltpu.make_async_copy(d_hbm, d_ref, load_s.at[5])
    feed_one.start()
    pieces_in = w_s.shape[1]
    depth = x_hbm.shape[1] // pieces_in

    def weight(i, c):
        src, dst = ((wq_hbm, wq_ref), (wk_hbm, wk_ref), (wv_hbm, wv_ref))[i]
        at = pl.ds(c * depth, depth)
        return pltpu.make_async_copy(src.at[at, :], dst.at[at, :], w_s.at[i, c])

    for i in range(3):
        for c in range(pieces_in):
            weight(i, c).start()
    loads = [
        pltpu.make_async_copy(src, dst, load_s.at[i])
        for i, (src, dst) in enumerate(
            ((ck_hbm, ck_ref), (cv_hbm, cv_ref), (dk_hbm, dk_ref), (dv_hbm, dv_ref))
        )
    ]
    for load in loads:
        load.start()
    load_out = pltpu.make_async_copy(wo_hbm, wo_ref, load_s.at[6])
    load_out.start()

    barrier = pltpu.get_barrier_semaphore()
    for s in range(1, n):
        pl.semaphore_signal(barrier, inc=1, device_id={"kv": lax.rem(me + s, n)}, device_id_type=MESH)
    for s in range(1, tp):
        pl.semaphore_signal(barrier, inc=1, device_id={"tp": lax.rem(mine + s, tp)}, device_id_type=MESH)

    feed_one.wait()
    feed.wait()
    gain_in = in_gain_ref[...].astype(jnp.float32)[None, :]
    xs[pl.ds(0, rows), :] = rms_scaled(x_ref[...], gain_in).astype(jnp.bfloat16)
    line = lax.broadcasted_iota(jnp.int32, (16, x_ref.shape[1]), 0)
    single = jnp.zeros((16, x_ref.shape[1]), jnp.float32)
    for b in range(seqs):
        single = jnp.where(line == b, rms_scaled(d_ref[b : b + 1, :], gain_in), single)
    xs[pl.ds(rows, 16), :] = single.astype(jnp.bfloat16)

    def projected(i):
        total = None
        for c in range(pieces_in):
            weight(i, c).wait()
            at = pl.ds(c * depth, depth)
            part = dot(xs[:, at], (wq_ref, wk_ref, wv_ref)[i][at, :])
            total = part if total is None else total + part
        return total.astype(jnp.bfloat16)

    projection = projected(0)
    q_ref[...] = projection[0:rows]
    dq_ref[...] = projection[rows:]
    pl.semaphore_wait(barrier, n - 1 + tp - 1)

    def remote(src, dst, ss, rs, peer, axis="kv"):
        return pltpu.make_async_remote_copy(
            src_ref=src, dst_ref=dst, send_sem=ss, recv_sem=rs,
            device_id={axis: peer}, device_id_type=MESH,
        )

    def q_plane(s):
        return remote(q_ref, qg.at[me], q_zs.at[s], q_rs.at[me], target(s) * ny + y)

    def q_column(k):
        return remote(q_ref, qg.at[me], q_ys.at[k], q_rs.at[me], z * ny + other(k))

    def q_block(c, s, k):
        return remote(qg.at[c], qg.at[c], q_fs.at[s, k], q_rs.at[c], z * ny + other(k))

    for s in range(1, nz):
        q_plane(s).start()
    for k in range(1, ny):
        q_column(k).start()
    qg[me] = q_ref[...]

    projection = projected(1)
    k_ref[...] = projection[0:rows]
    dec_k_ref[...] = projection[rows : rows + seqs]
    projection = projected(2)
    v_ref[...] = projection[0:rows]
    dec_v_ref[...] = projection[rows : rows + seqs]
    keeps = [
        pltpu.make_async_copy(k_ref, k_out, keep_s.at[0]),
        pltpu.make_async_copy(v_ref, v_out, keep_s.at[1]),
    ]
    for keep in keeps:
        keep.start()
    short = spread_matrix(rows)
    for h in range(heads):
        kvb[h, 0:rows, :] = dot(short, k_ref[:, head_cols(h)]).astype(jnp.bfloat16)
        kvb[h, rows : 2 * rows, :] = jnp.transpose(dot(short, v_ref[:, head_cols(h)])).astype(jnp.bfloat16)

    def kv_plane(t):
        return remote(kvb.at[t % heads], kvg.at[me], kv_zs.at[t], kv_rs.at[me], t * ny + y)

    def kv_column(k):
        return remote(kvb.at[my_head], kvg.at[me], kv_ys.at[k], kv_rs.at[me], z * ny + other(k))

    def kv_block(c, s, k):
        return remote(kvg.at[c], kvg.at[c], kv_fs.at[s, k], kv_rs.at[c], z * ny + other(k))

    for t in range(nz):
        pl.when(z != t)(lambda t=t: kv_plane(t).start())
    for k in range(1, ny):
        kv_column(k).start()
    kvg[me] = kvb[my_head]

    loads[0].wait()
    loads[1].wait()
    run = cache_rows // 8
    tiles = run // 32
    wide = spread_matrix(256)
    for t in range(tiles):
        def strip(ref):
            return jnp.concatenate([ref[pl.ds(s * run + t * 32, 32), :] for s in range(8)], axis=0)
        keys = dot(wide, strip(ck_ref)).astype(jnp.bfloat16)
        values = dot(wide, strip(cv_ref))
        for h in range(heads):
            kp[h, t * 256 : t * 256 + 256, :] = keys[:, h * HEAD : h * HEAD + HEAD]
            vt[h, :, t * 256 : t * 256 + 256] = jnp.transpose(
                values[:, h * HEAD : h * HEAD + HEAD]
            ).astype(jnp.bfloat16)
    row = lax.broadcasted_iota(jnp.int32, (cache_rows, 128), 0)
    valid = me * cache_rows + lax.rem(row, 8) * run + row // 8 < ctx_ref[0]
    for h in range(heads):
        tab[h] = jnp.where(valid, off_ref[mine * heads + h] * LOG2E, HIDDEN)

    loads[2].wait()
    loads[3].wait()
    chunk = 256 if slots % 256 == 0 else 128
    suffix = suffix_matrix(chunk)
    hrow = lax.broadcasted_iota(jnp.int32, (8, width), 0)
    hcol = lax.broadcasted_iota(jnp.int32, (8, width), 1) // HEAD
    own_head = hrow == hcol
    head_row = lax.broadcasted_iota(jnp.int32, (8, chunk), 0)
    spot = lax.broadcasted_iota(jnp.int32, (8, chunk), 1)
    offsets = jnp.zeros((8, chunk), jnp.float32)
    for h in range(heads):
        offsets = jnp.where(head_row == h, off_ref[mine * heads + h], offsets)
    dec_rows = jnp.zeros((16, width), jnp.float32)
    for b in range(seqs):
        query = jnp.where(own_head, dq_ref[b : b + 1, :].astype(jnp.float32), 0.0).astype(jnp.bfloat16)
        out, unused = cached_terms(
            query,
            lambda start: dk_ref[b, pl.ds(start, chunk), :],
            lambda start: dv_ref[b, pl.ds(start, chunk), :],
            lambda start: jnp.where(spot + start < len_ref[b], offsets, HIDDEN),
            slots, chunk, suffix, scale,
        )
        line = jnp.sum(jnp.where(own_head, out, 0.0), axis=0, keepdims=True)
        place = lax.broadcasted_iota(jnp.int32, (16, width), 0)
        dec_rows = jnp.where(place == b, line, dec_rows)
    att[pl.ds(rows, 16), :] = dec_rows.astype(att.dtype)

    def forward(block, s):
        c = source(s) * ny + y
        block(c, s, 0).wait_recv()
        for k in range(1, ny):
            block(c, s, k).start()

    def piece_out(j):
        return remote(ps.at[j], pr.at[my_head], p_s.at[j], p_r.at[my_head], (my_part + halves * j) * ny + y)

    def piece_total(j):
        return remote(pt.at[j], ptr.at[my_head], pt_s.at[j], pt_r.at[my_head], (my_part + halves * j) * ny + y)

    def pieces():
        for k in range(1, ny):
            for u in range(nz):
                kv_block(u * ny + other(k), 0, 0).wait_recv()
        cols = pl.ds(pl.multiple_of(my_head * HEAD, HEAD), HEAD)
        for j in range(heads):
            qp[j * rows : j * rows + rows, :] = qg[(my_part + halves * j) * ny + y, :, cols]
        pacc[...] = jnp.zeros_like(pacc)
        plat[...] = jnp.ones_like(plat)
        lane = lax.broadcasted_iota(jnp.int32, (8, 128), 1)
        first = lax.broadcasted_iota(jnp.int32, (8, 128), 0) * (rows // 8)
        off = off_ref[mine * heads + my_head] * LOG2E

        def block(i, carry):
            c = n - 1 - i
            pz[...] = dot_t(kvg[c, 0:rows, :], qp[...])

            def score(v, g):
                seen = c * rows + first + v < ((my_part + halves * g) * ny + y) * rows + lane
                return jnp.where(seen, pz[v * 8 : v * 8 + 8, g * 128 : g * 128 + 128] * scale2 + off, HIDDEN)

            def store(v, g, w):
                pz[v * 8 : v * 8 + 8, g * 128 : g * 128 + 128] = w

            left = break_sticks(score, store, rows // 8, heads)
            factors = [later_sublanes(x) for x in left]
            factor = jnp.concatenate(factors, axis=1)
            w = pz[...].reshape(rows // 8, 8, heads * rows) * factor[None]
            w = w.reshape(rows, heads * rows).astype(jnp.bfloat16)
            pacc[...] += dot(kvg[c, rows : 2 * rows, :], w) * plat[0:1, :]
            whole = (factor * jnp.concatenate(left, axis=1))[0:1, :]
            plat[...] = plat[...] * whole
            return carry

        lax.fori_loop(0, n, block, 0)
        for j in range(heads):
            owner = my_part + halves * j
            ps[j] = pacc[:, j * rows : j * rows + rows].astype(jnp.bfloat16)
            pt[j] = plat[:, j * rows : j * rows + rows]

            @pl.when(owner != z)
            def _():
                piece_out(j).start()
                piece_total(j).start()

            @pl.when(owner == z)
            def _():
                pr[my_head] = ps[j]
                ptr[my_head] = pt[j]

    def o_column(u, s, k):
        return remote(obuf.at[u, other(k)], oy.at[u, y], oy_s.at[s, k], oy_r.at[u, y], z * ny + other(k))

    def t_column(u, s, k):
        return remote(tbuf.at[u, other(k)], ty.at[u, y], ty_s.at[s, k], ty_r.at[u, y], z * ny + other(k))

    def o_from(u, c):
        return remote(obuf.at[u, c], oy.at[u, c], oy_s.at[0, 0], oy_r.at[u, c], z * ny + other(1))

    def t_from(u, c):
        return remote(tbuf.at[u, c], ty.at[u, c], ty_s.at[0, 0], ty_r.at[u, c], z * ny + other(1))

    def compute(u):
        totals = [jnp.ones((8, 128), jnp.float32) for _ in range(ny)]
        place = lax.broadcasted_iota(jnp.int32, (8, 128), 0)
        for h in range(heads):
            q = qg[pl.ds(u * ny, ny), :, head_cols(h)].reshape(ny * rows, HEAD)
            zbuf[h] = dot_t(kp[h], q)

            def score(v, g):
                at = slice(v * 8, v * 8 + 8)
                return zbuf[h, at, g * 128 : g * 128 + 128] * scale2 + tab[h, at, :]

            def store(v, g, w):
                zbuf[h, v * 8 : v * 8 + 8, g * 128 : g * 128 + 128] = w

            left = break_sticks(score, store, run, ny)
            factors = [later_sublanes(x) for x in left]
            factor = jnp.concatenate(factors, axis=1)
            w = zbuf[h].reshape(run, 8, ny * rows) * factor[None]
            out = dot(vt[h], w.reshape(cache_rows, ny * rows).astype(jnp.bfloat16))
            for g in range(ny):
                part = out[:, g * rows : g * rows + rows]
                own[u, g, head_cols(h), :] = part
                obuf[u, g, head_cols(h), :] = part.astype(jnp.bfloat16)
                totals[g] = jnp.where(place == h, (factors[g] * left[g])[0:1, :], totals[g])
        for g in range(ny):
            tbuf[u, g] = totals[g]
        ty[u, y] = tbuf[u, y]

    def o_plane(u, s):
        return remote(zs.at[u], zr.at[z], oz_s.at[s], oz_r.at[z], u * ny + y)

    def t_plane(u, s):
        return remote(zt.at[u], ztr.at[z], tz_s.at[s], tz_r.at[z], u * ny + y)

    def combine(s):
        u = source(s)
        mix[y] = own[u, y]
        for k in range(1, ny):
            o_from(u, other(k)).wait_recv()
            t_from(u, other(k)).wait_recv()
            mix[other(k)] = oy[u, other(k)].astype(jnp.float32)
        later = jnp.ones((8, 128), jnp.float32)
        factors = []
        for c in reversed(range(ny)):
            factors.append(later)
            later = later * ty[u, c]
        for h in range(heads):
            total = jnp.zeros((HEAD, rows), jnp.float32)
            for c in range(ny):
                total += mix[c, head_cols(h), :] * factors[ny - 1 - c][h : h + 1, :]
            zs[u, head_cols(h), :] = total.astype(jnp.bfloat16)

            @pl.when(u == z)
            def _():
                zmix[z, head_cols(h), :] = total

        zt[u] = later

        @pl.when(u == z)
        def _():
            ztr[z] = later

        @pl.when(u != z)
        def _():
            o_plane(u, s).start()
            t_plane(u, s).start()

    def step(s, carry):
        u = source(s)
        pl.when(s + 1 < nz)(lambda: forward(q_block, s + 1))

        @pl.when(s == nz - 1)
        def _():
            for r in range(1, nz):
                forward(kv_block, r)

        for k in range(1, ny):
            q_block(u * ny + other(k), 0, 0).wait_recv()
        compute(u)
        for k in range(1, ny):
            o_column(u, s, k).start()
            t_column(u, s, k).start()
        pl.when(s > 0)(lambda: combine(s - 1))
        return carry

    lax.fori_loop(0, nz, step, 0)
    pieces()
    combine(nz - 1)

    for h in range(heads):
        plane = lax.rem(z, halves) * heads + h

        @pl.when(plane != z)
        def _():
            remote(ps.at[0], pr.at[h], p_s.at[0], p_r.at[h], plane * ny + y).wait_recv()
            remote(pt.at[0], ptr.at[h], pt_s.at[0], pt_r.at[h], plane * ny + y).wait_recv()

    for s in range(1, nz):
        u = source(s)
        remote(zs.at[u], zr.at[u], oz_s.at[s], oz_r.at[u], u * ny + y).wait_recv()
        remote(zt.at[u], ztr.at[u], tz_s.at[s], tz_r.at[u], u * ny + y).wait_recv()
        zmix[u] = zr[u].astype(jnp.float32)

    later = jnp.ones((8, 128), jnp.float32)
    factors = []
    for c in reversed(range(nz)):
        factors.append(later)
        later = later * ztr[c]
    for h in range(heads):
        total = jnp.zeros((HEAD, rows), jnp.float32)
        for c in range(nz):
            total += zmix[c, head_cols(h), :] * factors[nz - 1 - c][h : h + 1, :]
        total = total * ptr[h, 0:1, :] + pr[h].astype(jnp.float32)
        att[pl.ds(0, rows), head_cols(h)] = jnp.transpose(total).astype(att.dtype)

    core = lax.rem(mine, 2)
    sibling = mine + 1 - 2 * core

    def across(s):
        return remote(att, attg.at[mine], a_s.at[s], a_r.at[mine], lax.rem(mine + 2 * s, tp), "tp")

    def beside(c):
        return remote(attg.at[c], attg.at[c], b_s.at[c], a_r.at[c], sibling, "tp")

    for s in range(1, tp // 2):
        across(s).start()
    attg[mine] = att[...]
    remote(att, attg.at[mine], a_s.at[0], a_r.at[mine], sibling, "tp").start()

    for s in range(1, nz):
        q_plane(s).wait_send()
        u = source(s)
        c = u * ny + y
        o_plane(u, s).wait_send()
        t_plane(u, s).wait_send()
        for k in range(1, ny):
            q_block(c, s, k).wait_send()
            kv_block(c, s, k).wait_send()
    for t in range(nz):
        pl.when(z != t)(lambda t=t: kv_plane(t).wait_send())
    for k in range(1, ny):
        q_column(k).wait_send()
        kv_column(k).wait_send()
        for s in range(nz):
            o_column(source(s), s, k).wait_send()
            t_column(source(s), s, k).wait_send()
    for j in range(heads):

        @pl.when(my_part + halves * j != z)
        def _():
            piece_out(j).wait_send()
            piece_total(j).wait_send()

    for s in range(1, tp // 2):
        c = lax.rem(mine + tp - 2 * s, tp)
        beside(c).wait_recv()
        beside(c).start()
    for s in range(tp // 2):
        beside(lax.rem(sibling + 2 * s, tp)).wait_recv()
    remote(att, attg.at[mine], a_s.at[0], a_r.at[mine], sibling, "tp").wait_send()
    for s in range(1, tp // 2):
        across(s).wait_send()
        beside(lax.rem(mine + tp - 2 * s, tp)).wait_send()
    square = jnp.zeros((att.shape[0], 1), jnp.float32)
    for t in range(tp):
        values = attg[t].astype(jnp.float32)
        square += jnp.sum(values * values, axis=-1, keepdims=True)
    inverse = lax.rsqrt(square / (tp * width) + EPS)
    gain_out = gain_ref[...].astype(jnp.float32)[None, :]
    for t in range(tp):
        cols = slice(t * width, t * width + width)
        normed[:, cols] = (attg[t].astype(jnp.float32) * inverse * gain_out[:, cols]).astype(jnp.bfloat16)
    load_out.wait()
    result = dot(normed[...], wo_ref[...]).astype(jnp.bfloat16)
    out_ref[...] = result[0:rows]
    dec_ref[...] = result[rows : rows + seqs]
    for keep in keeps:
        keep.wait()


def deliver_kernel(*refs):
    sems = refs[-1]
    count = sems.shape[1]
    sources, targets, held = refs[:count], refs[count : 2 * count], refs[2 * count : 3 * count]
    taken = [pltpu.make_async_copy(sources[i], held[i], sems.at[0, i]) for i in range(count)]
    given = [pltpu.make_async_copy(held[i], targets[i], sems.at[1, i]) for i in range(count)]
    for i in range(count):
        taken[i].start()
    for i in range(count):
        taken[i].wait()
        given[i].start()
    for i in range(count):
        given[i].wait()


def body(
    piece_tokens, decode_tokens, norm_gain, w_query, w_key, w_value, score_offset, context_length,
    prompt_keys, prompt_values, decode_keys, decode_values, decoding_cache_length, out_gain, w_out,
):
    n, tp = lax.axis_size("kv"), lax.axis_size("tp")
    nz, ny = grid_of(n)
    rows, model = piece_tokens.shape
    width = w_query.shape[1]
    seqs = decode_keys.shape[0]
    heads = width // HEAD
    assert nz % heads == 0 and tp % 2 == 0
    cache_rows = prompt_keys.shape[0]
    vmem = pl.BlockSpec(memory_space=pltpu.VMEM)
    smem = pl.BlockSpec(memory_space=pltpu.SMEM)
    hbm = pl.BlockSpec(memory_space=pl.ANY)
    dma = pltpu.SemaphoreType.DMA

    def half(*shape):
        return pltpu.VMEM(shape, jnp.bfloat16)

    def full(*shape):
        return pltpu.VMEM(shape, jnp.float32)

    def result(*shape):
        return jax.ShapeDtypeStruct(shape, jnp.bfloat16)

    results = pl.pallas_call(
        functools.partial(attention_kernel, nz, ny, tp, heads),
        out_shape=(
            result(rows, w_out.shape[1]), result(seqs, w_out.shape[1]), result(rows, width), result(rows, width),
            result(seqs, width), result(seqs, width),
        ),
        in_specs=[hbm] * 10 + [vmem] * 2 + [smem] * 3,
        out_specs=(vmem, vmem, hbm, hbm, vmem, vmem),
        scratch_shapes=[
            half(rows, model), half(seqs, model), half(model, width), half(model, width), half(model, width),
            half(*prompt_keys.shape), half(*prompt_values.shape), half(*decode_keys.shape), half(*decode_values.shape),
            half(*w_out.shape),
            half(rows + 16, model), half(rows, width), half(rows, width), half(rows, width), half(16, width),
            half(rows + 16, tp * width),
            half(n, rows, width), half(heads, cache_rows, HEAD), half(heads, HEAD, cache_rows),
            full(heads, cache_rows, 128), full(heads, cache_rows, ny * rows),
            full(nz, ny, width, rows), half(nz, ny, width, rows), full(nz, ny, 8, 128),
            half(nz, ny, width, rows), full(nz, ny, 8, 128), full(ny, width, rows),
            half(nz, width, rows), full(nz, 8, 128), half(nz, width, rows), full(nz, 8, 128),
            full(nz, width, rows),
            half(heads, 2 * rows, HEAD), half(n, 2 * rows, HEAD), half(heads * rows, HEAD),
            full(rows, heads * rows), full(HEAD, heads * rows), full(8, heads * rows),
            half(heads, HEAD, rows), full(heads, 8, 128), half(heads, HEAD, rows), full(heads, 8, 128),
            half(rows + 16, width), half(tp, rows + 16, width),
            dma((ny,)), dma((nz,)), dma((nz, ny)), dma((n,)),
            dma((nz,)), dma((ny,)), dma((nz, ny)), dma((n,)),
            dma((nz, ny)), dma((nz, ny)), dma((nz, ny)), dma((nz, ny)),
            dma((nz,)), dma((nz,)), dma((nz,)), dma((nz,)),
            dma((heads,)), dma((heads,)), dma((heads,)), dma((heads,)),
            dma((tp,)), dma((tp,)), dma((tp,)), dma((7,)), dma((3, 8)), dma((2,)),
        ],
        compiler_params=pltpu.CompilerParams(
            collective_id=0, has_side_effects=True, vmem_limit_bytes=60 * 1024 * 1024
        ),
        name="attend",
    )(
        piece_tokens, decode_tokens, w_query, w_key, w_value, prompt_keys, prompt_values, decode_keys, decode_values,
        w_out, norm_gain, out_gain, score_offset, context_length, decoding_cache_length,
    )
    kinds = [jax.ShapeDtypeStruct(r.shape, r.dtype) for r in results]
    return pl.pallas_call(
        deliver_kernel,
        out_shape=kinds,
        in_specs=[hbm] * len(kinds),
        out_specs=[hbm] * len(kinds),
        scratch_shapes=[pltpu.VMEM(k.shape, k.dtype) for k in kinds] + [dma((2, len(kinds)))],
        name="deliver",
    )(*results)


def solution(mesh):
    in_specs = (
        P("kv", None),
        P("kv", None),
        P(),
        P(None, "tp"),
        P(None, "tp"),
        P(None, "tp"),
        P(),
        P(),
        P("kv", "tp"),
        P("kv", "tp"),
        P("kv", None, "tp"),
        P("kv", None, "tp"),
        P("kv"),
        P(),
        P(None, "tp"),
    )
    out_specs = (
        P("kv", "tp"),
        P("kv", "tp"),
        P("kv", "tp"),
        P("kv", "tp"),
        P("kv", "tp"),
        P("kv", "tp"),
    )
    return jax.shard_map(body, mesh=mesh, in_specs=in_specs, out_specs=out_specs, check_vma=False)
```

```python
import functools
import math

import jax
import jax.numpy as jnp
from jax import lax
from jax.experimental import pallas as pl
from jax.experimental.pallas import tpu as pltpu
from jax.sharding import PartitionSpec as P

HEAD = 128
EPS = 1e-06
HIDDEN = -1e30
LAG = 3
KV_AT = 2
LOG2E = 1.4426950408889634
MESH = pl.DeviceIdType.MESH


def rms_scaled(rows, gain):
    values = rows.astype(jnp.float32)
    inverse = lax.rsqrt(jnp.mean(values * values, axis=-1, keepdims=True) + EPS)
    return values * inverse * gain


def suffix_matrix(size):
    row = lax.broadcasted_iota(jnp.int32, (size, size), 0)
    column = lax.broadcasted_iota(jnp.int32, (size, size), 1)
    return jnp.where(row >= column, 1.0, 0.0).astype(jnp.bfloat16)


def spread_matrix(size):
    run = size // 8
    row = lax.broadcasted_iota(jnp.int32, (size, size), 0)
    column = lax.broadcasted_iota(jnp.int32, (size, size), 1)
    hit = (row // 8 == column % run) & (row % 8 == column // run)
    return jnp.where(hit, 1.0, 0.0).astype(jnp.bfloat16)


def dot_t(a, b):
    return lax.dot_general(a, b, (((1,), (1,)), ((), ())), preferred_element_type=jnp.float32)


def dot(a, b):
    return jnp.dot(a, b, preferred_element_type=jnp.float32)


def suffix_keep(z, suffix):
    keep = -(jnp.maximum(z, 0.0) + jnp.log(1.0 + jnp.exp(-jnp.abs(z))))
    high = keep.astype(jnp.bfloat16)
    low = (keep - high.astype(jnp.float32)).astype(jnp.bfloat16)
    return dot(high, suffix) + dot(low, suffix)


def cached_terms(query, key_of, value_of, bias_of, total_keys, chunk, suffix, scale):
    later = None
    out = None
    for start in reversed(range(0, total_keys, chunk)):
        z = dot_t(query, key_of(start)) * scale + bias_of(start)
        inner = suffix_keep(z, suffix)
        exponent = z + inner if later is None else z + inner + later
        weight = jnp.exp(exponent).astype(jnp.bfloat16)
        part = dot(weight, value_of(start))
        out = part if out is None else out + part
        later = inner[:, 0:1] if later is None else later + inner[:, 0:1]
    return out, later


def grid_of(n):
    columns = max(d for d in range(1, math.isqrt(n) + 1) if n % d == 0)
    return n // columns, columns


def later_sublanes(runs):
    place = lax.broadcasted_iota(jnp.int32, runs.shape, 0)

    def up(x, k):
        return jnp.where(place < 8 - k, pltpu.roll(x, 8 - k, 0), 1.0)

    x = up(runs, 1)
    x = x * up(x, 1)
    x = x * up(x, 2)
    return x * up(x, 4)


def break_sticks(score, store, steps, groups):
    left = [jnp.ones((8, 128), jnp.float32) for _ in range(groups)]
    for v in reversed(range(steps)):
        for g in range(groups):
            e = jnp.exp2(jnp.minimum(score(v, g), 126.0))
            left[g] = left[g] * (1.0 / (1.0 + e))
            store(v, g, e * left[g])
    return left


def attention_kernel(
    nz, ny, tp, heads, parts, x_hbm, d_hbm, wq_hbm, wk_hbm, wv_hbm, ck_hbm, cv_hbm, dk_hbm, dv_hbm, wo_hbm,
    in_gain_ref, gain_ref, off_ref, ctx_ref, len_ref, out_ref, dec_ref, k_out, v_out, dec_k_ref, dec_v_ref,
    x_ref, d_ref, wq_ref, wk_ref, wv_ref, ck_ref, cv_ref, dk_ref, dv_ref, wo_ref,
    xs, q_ref, k_ref, v_ref, dq_ref, normed,
    qg, kp, vt, tab, zbuf, own, obuf, tbuf, oy, ty, mix, pair, zs, zt, zr, ztr, zmix, zmine,
    kvb, kvg, qp, pz, pout, pacc, plat, ps, pt, pr, ptr, att, attg,
    q_ys, q_zs, q_fs, q_rs, kv_zs, kv_ys, kv_fs, kv_rs, oy_s, oy_r, ty_s, ty_r, oz_s, oz_r, tz_s, tz_r,
    p_s, p_r, pt_s, pt_r, a_s, a_r, b_s, load_s, w_s, keep_s, q_hs,
):
    n = nz * ny
    me = lax.axis_index("kv")
    mine = lax.axis_index("tp")
    z = me // ny
    y = lax.rem(me, ny)
    rows = x_hbm.shape[0]
    width = heads * HEAD
    share = heads // parts
    band = share * HEAD
    cache_rows = ck_ref.shape[0]
    seqs, slots = dk_hbm.shape[0], dk_hbm.shape[1]
    scale = HEAD ** (-0.5)
    scale2 = scale * LOG2E
    halves = nz // heads
    my_head = lax.rem(z, heads)
    my_part = z // heads
    bits = nz.bit_length() - 1
    far = nz == 4

    def source(s):
        total = 0
        for b in range(bits):
            total += lax.rem(lax.rem(z // (1 << b), 2) + lax.rem(s // (1 << b), 2), 2) * (1 << b)
        return total

    def other(k):
        return lax.rem(y + k, ny)

    def head_cols(h):
        return pl.ds(h * HEAD, HEAD)

    feed = pltpu.make_async_copy(x_hbm, x_ref, load_s.at[4])
    feed.start()
    feed_one = pltpu.make_async_copy(d_hbm, d_ref, load_s.at[5])
    feed_one.start()
    pieces_in = w_s.shape[1]
    depth = x_hbm.shape[1] // pieces_in

    def weight(i, c):
        src, dst = ((wq_hbm, wq_ref), (wk_hbm, wk_ref), (wv_hbm, wv_ref))[i]
        at = pl.ds(c * depth, depth)
        return pltpu.make_async_copy(src.at[at, :], dst.at[at, :], w_s.at[i, c])

    for c in range(pieces_in):
        weight(0, c).start()
    loads = [
        pltpu.make_async_copy(src, dst, load_s.at[i])
        for i, (src, dst) in enumerate(
            ((ck_hbm, ck_ref), (cv_hbm, cv_ref), (dk_hbm, dk_ref), (dv_hbm, dv_ref))
        )
    ]
    loads[0].start()
    loads[1].start()
    for i in range(1, 3):
        for c in range(pieces_in):
            weight(i, c).start()
    loads[2].start()
    loads[3].start()
    load_out = pltpu.make_async_copy(wo_hbm, wo_ref, load_s.at[6])
    load_out.start()

    barrier = pltpu.get_barrier_semaphore()
    for s in range(1, n):
        pl.semaphore_signal(barrier, inc=1, device_id={"kv": lax.rem(me + s, n)}, device_id_type=MESH)
    for s in range(1, tp):
        pl.semaphore_signal(barrier, inc=1, device_id={"tp": lax.rem(mine + s, tp)}, device_id_type=MESH)

    feed_one.wait()
    feed.wait()
    gain_in = in_gain_ref[...].astype(jnp.float32)[None, :]
    xs[pl.ds(0, rows), :] = rms_scaled(x_ref[...], gain_in).astype(jnp.bfloat16)
    line = lax.broadcasted_iota(jnp.int32, (16, x_ref.shape[1]), 0)
    single = jnp.zeros((16, x_ref.shape[1]), jnp.float32)
    for b in range(seqs):
        single = jnp.where(line == b, rms_scaled(d_ref[b : b + 1, :], gain_in), single)
    xs[pl.ds(rows, 16), :] = single.astype(jnp.bfloat16)

    def projected(i):
        total = None
        for c in range(pieces_in):
            weight(i, c).wait()
            at = pl.ds(c * depth, depth)
            part = dot(xs[:, at], (wq_ref, wk_ref, wv_ref)[i][at, :])
            total = part if total is None else total + part
        return total.astype(jnp.bfloat16)

    projection = projected(0)
    for p in range(parts):
        q_ref[p] = projection[0:rows, p * band : p * band + band]
    dq_ref[...] = projection[rows:]
    pl.semaphore_wait(barrier, n - 1 + tp - 1)

    def remote(src, dst, ss, rs, peer, axis="kv"):
        return pltpu.make_async_remote_copy(
            src_ref=src, dst_ref=dst, send_sem=ss, recv_sem=rs,
            device_id={axis: peer}, device_id_type=MESH,
        )

    def q_plane(s, p):
        return remote(q_ref.at[p], qg.at[me, p], q_zs.at[s, p], q_rs.at[me, p], source(s) * ny + y)

    def q_column(k, p):
        return remote(q_ref.at[p], qg.at[me, p], q_ys.at[k, p], q_rs.at[me, p], z * ny + other(k))

    def q_block(c, s, p, k):
        return remote(qg.at[c, p], qg.at[c, p], q_fs.at[s, p, k], q_rs.at[c, p], z * ny + other(k))

    def q_relay(s, p):
        c = source(s) * ny + y
        return remote(qg.at[c, p], qg.at[c, p], q_hs.at[p], q_rs.at[c, p], source(1) * ny + y)

    direct = (2, 1) if far else (1,)
    for s in direct:
        for p in range(parts):
            q_plane(s, p).start()
    for k in range(1, ny):
        for p in range(parts):
            q_column(k, p).start()
    qg[me] = q_ref[...]

    loads[0].wait()
    loads[1].wait()
    run = cache_rows // 8
    tiles = run // 32
    wide = spread_matrix(256)
    for t in range(tiles):
        def strip(ref):
            return jnp.concatenate([ref[pl.ds(s * run + t * 32, 32), :] for s in range(8)], axis=0)
        keys = dot(wide, strip(ck_ref)).astype(jnp.bfloat16)
        values = dot(wide, strip(cv_ref))
        for h in range(heads):
            kp[h, t * 256 : t * 256 + 256, :] = keys[:, h * HEAD : h * HEAD + HEAD]
            vt[h, :, t * 256 : t * 256 + 256] = jnp.transpose(
                values[:, h * HEAD : h * HEAD + HEAD]
            ).astype(jnp.bfloat16)
    row = lax.broadcasted_iota(jnp.int32, (cache_rows, 128), 0)
    valid = me * cache_rows + lax.rem(row, 8) * run + row // 8 < ctx_ref[0]
    for h in range(heads):
        tab[h] = jnp.where(valid, off_ref[mine * heads + h] * LOG2E, HIDDEN)

    def forward_q(s, p):
        c = source(s) * ny + y
        q_block(c, s, p, 0).wait_recv()
        if far and s == 2:
            q_relay(s, p).start()
        for k in range(1, ny):
            q_block(c, s, p, k).start()

    def forward_kv(s):
        c = source(s) * ny + y
        kv_block(c, s, 0).wait_recv()
        for k in range(1, ny):
            kv_block(c, s, k).start()

    def piece_out(j):
        return remote(ps.at[j], pr.at[my_head], p_s.at[j], p_r.at[my_head], (my_part + halves * j) * ny + y)

    def piece_total(j):
        return remote(pt.at[j], ptr.at[my_head], pt_s.at[j], pt_r.at[my_head], (my_part + halves * j) * ny + y)

    def pieces():
        for k in range(1, ny):
            for u in range(nz):
                kv_block(u * ny + other(k), 0, 0).wait_recv()
        cols = pl.ds(pl.multiple_of(lax.rem(my_head, share) * HEAD, HEAD), HEAD)
        for j in range(heads):
            qp[j * rows : j * rows + rows, :] = qg[(my_part + halves * j) * ny + y, my_head // share, :, cols]
        pacc[...] = jnp.zeros_like(pacc)
        plat[...] = jnp.ones_like(plat)
        lane = lax.broadcasted_iota(jnp.int32, (8, 128), 1)
        first = lax.broadcasted_iota(jnp.int32, (8, 128), 0) * (rows // 8)
        off = off_ref[mine * heads + my_head] * LOG2E

        batch = 4 if n % 4 == 0 else 1

        def block(c, slot):
            pz[slot] = dot_t(kvg[c, 0:rows, :], qp[...])

            def score(v, g):
                seen = c * rows + first + v < ((my_part + halves * g) * ny + y) * rows + lane
                at = pz[slot, v * 8 : v * 8 + 8, g * 128 : g * 128 + 128]
                return jnp.where(seen, at * scale2 + off, HIDDEN)

            def store(v, g, w):
                pz[slot, v * 8 : v * 8 + 8, g * 128 : g * 128 + 128] = w

            left = break_sticks(score, store, rows // 8, heads)
            factors = [later_sublanes(x) for x in left]
            factor = jnp.concatenate(factors, axis=1)
            w = pz[slot].reshape(rows // 8, 8, heads * rows) * factor[None]
            w = w.reshape(rows, heads * rows).astype(jnp.bfloat16)
            pout[slot] = dot(kvg[c, rows : 2 * rows, :], w)
            return (factor * jnp.concatenate(left, axis=1))[0:1, :]

        def several(i, carry):
            wholes = [block(n - 1 - i * batch - slot, slot) for slot in range(batch)]
            later = plat[0:1, :]
            total = pacc[...]
            for slot in range(batch):
                total += pout[slot] * later
                later = later * wholes[slot]
            pacc[...] = total
            plat[...] = jnp.broadcast_to(later, plat.shape)
            return carry

        lax.fori_loop(0, n // batch, several, 0)
        for j in range(heads):
            owner = my_part + halves * j
            ps[j] = pacc[:, j * rows : j * rows + rows].astype(jnp.bfloat16)
            pt[j] = plat[:, j * rows : j * rows + rows]

            @pl.when(owner != z)
            def _():
                piece_out(j).start()
                piece_total(j).start()

            @pl.when(owner == z)
            def _():
                pr[my_head] = ps[j]
                ptr[my_head] = pt[j]

    def o_column(u, s, p, k):
        return remote(
            obuf.at[u, p, other(k)], oy.at[u, p, y], oy_s.at[s, p, k], oy_r.at[u, p, y], z * ny + other(k)
        )

    def t_column(u, s, p, k):
        return remote(
            tbuf.at[u, p, other(k)], ty.at[u, p, y], ty_s.at[s, p, k], ty_r.at[u, p, y], z * ny + other(k)
        )

    def o_from(u, p, c):
        return remote(obuf.at[u, p, c], oy.at[u, p, c], oy_s.at[0, p, 0], oy_r.at[u, p, c], z * ny + other(1))

    def t_from(u, p, c):
        return remote(tbuf.at[u, p, c], ty.at[u, p, c], ty_s.at[0, p, 0], ty_r.at[u, p, c], z * ny + other(1))

    def compute(u, p):
        totals = [jnp.ones((8, 128), jnp.float32) for _ in range(ny)]
        place = lax.broadcasted_iota(jnp.int32, (8, 128), 0)
        for h in range(share):
            head = p * share + h
            q = qg[pl.ds(u * ny, ny), p, :, head_cols(h)].reshape(ny * rows, HEAD)
            zbuf[h] = dot_t(kp[head], q)

            def score(v, g):
                at = slice(v * 8, v * 8 + 8)
                return zbuf[h, at, g * 128 : g * 128 + 128] * scale2 + tab[head, at, :]

            def store(v, g, w):
                zbuf[h, v * 8 : v * 8 + 8, g * 128 : g * 128 + 128] = w

            left = break_sticks(score, store, run, ny)
            factors = [later_sublanes(x) for x in left]
            factor = jnp.concatenate(factors, axis=1)
            w = zbuf[h].reshape(run, 8, ny * rows) * factor[None]
            out = dot(vt[head], w.reshape(cache_rows, ny * rows).astype(jnp.bfloat16))
            for g in range(ny):
                block = out[:, g * rows : g * rows + rows]
                own[u, p, g, head_cols(h), :] = block
                obuf[u, p, g, head_cols(h), :] = block.astype(jnp.bfloat16)
                totals[g] = jnp.where(place == h, (factors[g] * left[g])[0:1, :], totals[g])
        for g in range(ny):
            tbuf[u, p, g] = totals[g]
        ty[u, p, y] = tbuf[u, p, y]

    def o_plane(s, p):
        return remote(zs.at[s, p], zr.at[s - 1, p], oz_s.at[s, p], oz_r.at[s - 1, p], source(s) * ny + y)

    def t_plane(s, p):
        return remote(zt.at[s, p], ztr.at[s - 1, p], tz_s.at[s, p], tz_r.at[s - 1, p], source(s) * ny + y)

    even = lax.rem(z, 2) == 0
    one = jnp.ones((8, 128), jnp.float32)

    def combine(s, p):
        u = source(s)
        mix[y] = own[u, p, y]
        for k in range(1, ny):
            o_from(u, p, other(k)).wait_recv()
            t_from(u, p, other(k)).wait_recv()
            mix[other(k)] = oy[u, p, other(k)].astype(jnp.float32)
        later = one
        factors = []
        for c in reversed(range(ny)):
            factors.append(later)
            later = later * ty[u, p, c]
        for h in range(share):
            total = jnp.zeros((HEAD, rows), jnp.float32)
            for c in range(ny):
                total += mix[c, head_cols(h), :] * factors[ny - 1 - c][h : h + 1, :]
            pair[head_cols(h), :] = total

        @pl.when(s == 0)
        def _():
            zmix[p] = pair[...]
            zmine[p] = later

        @pl.when(s > 0)
        def _():
            zs[s, p] = pair[...].astype(jnp.bfloat16)
            zt[s, p] = later
            o_plane(s, p).start()
            t_plane(s, p).start()

    def unit(s, p):
        u = source(s)
        for k in range(1, ny):
            q_block(u * ny + other(k), 0, p, 0).wait_recv()
        compute(u, p)
        for k in range(1, ny):
            o_column(u, s, p, k).start()
            t_column(u, s, p, k).start()

    def place_of(t):
        i = t // parts
        turn = lax.rem(lax.rem(i, 2) + i // 2, 2) * 2 + i // 2 if far else i
        return turn, lax.rem(t, parts)

    def step(t, carry):
        unit(*place_of(t))
        pl.when(t >= LAG)(lambda: combine(*place_of(t - LAG)))
        return carry

    def first(t, carry):
        unit(0, t)
        if far:
            forward_q(2, t)
        return carry

    projection = projected(1)
    k_ref[...] = projection[0:rows]
    dec_k_ref[...] = projection[rows : rows + seqs]
    projection = projected(2)
    v_ref[...] = projection[0:rows]
    dec_v_ref[...] = projection[rows : rows + seqs]
    keeps = [
        pltpu.make_async_copy(k_ref, k_out, keep_s.at[0]),
        pltpu.make_async_copy(v_ref, v_out, keep_s.at[1]),
    ]
    for keep in keeps:
        keep.start()
    short = spread_matrix(rows)
    for h in range(heads):
        kvb[h, 0:rows, :] = dot(short, k_ref[:, head_cols(h)]).astype(jnp.bfloat16)
        kvb[h, rows : 2 * rows, :] = jnp.transpose(dot(short, v_ref[:, head_cols(h)])).astype(jnp.bfloat16)

    def kv_plane(t):
        return remote(kvb.at[t % heads], kvg.at[me], kv_zs.at[t], kv_rs.at[me], t * ny + y)

    def kv_column(k):
        return remote(kvb.at[my_head], kvg.at[me], kv_ys.at[k], kv_rs.at[me], z * ny + other(k))

    def kv_block(c, s, k):
        return remote(kvg.at[c], kvg.at[c], kv_fs.at[s, k], kv_rs.at[c], z * ny + other(k))

    for t in range(nz):
        pl.when(z != t)(lambda t=t: kv_plane(t).start())
    for k in range(1, ny):
        kv_column(k).start()
    kvg[me] = kvb[my_head]

    lax.fori_loop(0, parts, first, 0)
    for p in range(parts):
        forward_q(1, p)
    loads[2].wait()
    loads[3].wait()
    chunk = 256 if slots % 256 == 0 else 128
    suffix = suffix_matrix(chunk)
    hrow = lax.broadcasted_iota(jnp.int32, (8, width), 0)
    hcol = lax.broadcasted_iota(jnp.int32, (8, width), 1) // HEAD
    own_head = hrow == hcol
    head_row = lax.broadcasted_iota(jnp.int32, (8, chunk), 0)
    spot = lax.broadcasted_iota(jnp.int32, (8, chunk), 1)
    offsets = jnp.zeros((8, chunk), jnp.float32)
    for h in range(heads):
        offsets = jnp.where(head_row == h, off_ref[mine * heads + h], offsets)
    dec_rows = jnp.zeros((16, width), jnp.float32)
    for b in range(seqs):
        query = jnp.where(own_head, dq_ref[b : b + 1, :].astype(jnp.float32), 0.0).astype(jnp.bfloat16)
        out, unused = cached_terms(
            query,
            lambda start: dk_ref[b, pl.ds(start, chunk), :],
            lambda start: dv_ref[b, pl.ds(start, chunk), :],
            lambda start: jnp.where(spot + start < len_ref[b], offsets, HIDDEN),
            slots, chunk, suffix, scale,
        )
        line = jnp.sum(jnp.where(own_head, out, 0.0), axis=0, keepdims=True)
        place = lax.broadcasted_iota(jnp.int32, (16, width), 0)
        dec_rows = jnp.where(place == b, line, dec_rows)
    for p in range(parts):
        att[p, pl.ds(rows, 16), :] = dec_rows[:, p * band : p * band + band].astype(att.dtype)

    if far:
        for p in range(parts):
            forward_q(3, p)

    def later_step(t, carry):
        step(t, carry)

        @pl.when(t == parts + KV_AT)
        def _():
            for s in range(1, nz):
                forward_kv(s)

        return carry

    lax.fori_loop(parts, nz * parts, later_step, 0)
    pieces()

    def tail(t, carry):
        combine(*place_of(t))
        return carry

    lax.fori_loop(nz * parts - LAG, nz * parts, tail, 0)

    for h in range(heads):
        plane = lax.rem(z, halves) * heads + h

        @pl.when(plane != z)
        def _():
            remote(ps.at[0], pr.at[h], p_s.at[0], p_r.at[h], plane * ny + y).wait_recv()
            remote(pt.at[0], ptr.at[h], pt_s.at[0], pt_r.at[h], plane * ny + y).wait_recv()

    core = lax.rem(mine, 2)
    sibling = mine + 1 - 2 * core

    def across(s, p):
        return remote(att.at[p], attg.at[mine, p], a_s.at[s, p], a_r.at[mine, p], lax.rem(mine + 2 * s, tp), "tp")

    def aside(p):
        return remote(att.at[p], attg.at[mine, p], a_s.at[0, p], a_r.at[mine, p], sibling, "tp")

    def beside(c, p):
        return remote(attg.at[c, p], attg.at[c, p], b_s.at[c, p], a_r.at[c, p], sibling, "tp")

    for p in range(parts):
        for s in range(1, nz):
            o_plane(s, p).wait_recv()
            t_plane(s, p).wait_recv()
        mine_left, near_left = zmine[p], ztr[0, p]
        scales = [jnp.where(even, near_left, one), jnp.where(even, one, mine_left)]
        if far:
            low = z < 2
            beyond = jnp.where(low, ztr[1, p] * ztr[2, p], one)
            nearer = jnp.where(low, one, mine_left * near_left)
            scales = [x * beyond for x in scales]
            scales.append(jnp.where(even, ztr[2, p], one) * nearer)
            scales.append(jnp.where(even, one, ztr[1, p]) * nearer)
        for h in range(share):
            line = slice(h, h + 1)
            total = zmix[p, head_cols(h), :] * scales[0][line, :]
            for s in range(1, nz):
                total += zr[s - 1, p, head_cols(h), :].astype(jnp.float32) * scales[s][line, :]
            head = p * share + h
            total = total * ptr[head, 0:1, :] + pr[head].astype(jnp.float32)
            att[p, pl.ds(0, rows), head_cols(h)] = jnp.transpose(total).astype(att.dtype)
        for s in range(1, tp // 2):
            across(s, p).start()
        aside(p).start()
        attg[mine, p] = att[p]

    for p in range(parts):
        for s in direct:
            q_plane(s, p).wait_send()
        if far:
            q_relay(2, p).wait_send()
        for s in range(1, nz):
            o_plane(s, p).wait_send()
            t_plane(s, p).wait_send()
            for k in range(1, ny):
                q_block(source(s) * ny + y, s, p, k).wait_send()
        for k in range(1, ny):
            q_column(k, p).wait_send()
            for s in range(nz):
                o_column(source(s), s, p, k).wait_send()
                t_column(source(s), s, p, k).wait_send()
    for s in range(1, nz):
        for k in range(1, ny):
            kv_block(source(s) * ny + y, s, k).wait_send()
    for k in range(1, ny):
        kv_column(k).wait_send()
    for t in range(nz):
        pl.when(z != t)(lambda t=t: kv_plane(t).wait_send())
    for j in range(heads):

        @pl.when(my_part + halves * j != z)
        def _():
            piece_out(j).wait_send()
            piece_total(j).wait_send()

    for p in range(parts):
        for s in range(1, tp // 2):
            c = lax.rem(mine + tp - 2 * s, tp)
            beside(c, p).wait_recv()
            beside(c, p).start()
    for p in range(parts):
        for s in range(tp // 2):
            beside(lax.rem(sibling + 2 * s, tp), p).wait_recv()
        aside(p).wait_send()
        for s in range(1, tp // 2):
            across(s, p).wait_send()
            beside(lax.rem(mine + tp - 2 * s, tp), p).wait_send()
    square = jnp.zeros((rows + 16, 1), jnp.float32)
    for t in range(tp):
        for p in range(parts):
            values = attg[t, p].astype(jnp.float32)
            square += jnp.sum(values * values, axis=-1, keepdims=True)
    inverse = lax.rsqrt(square / (tp * width) + EPS)
    gain_out = gain_ref[...].astype(jnp.float32)[None, :]
    for t in range(tp):
        for p in range(parts):
            cols = slice(t * width + p * band, t * width + p * band + band)
            normed[:, cols] = (attg[t, p].astype(jnp.float32) * inverse * gain_out[:, cols]).astype(jnp.bfloat16)
    load_out.wait()
    result = dot(normed[...], wo_ref[...]).astype(jnp.bfloat16)
    out_ref[...] = result[0:rows]
    dec_ref[...] = result[rows : rows + seqs]
    for keep in keeps:
        keep.wait()


def deliver_kernel(*refs):
    sems = refs[-1]
    count = sems.shape[1]
    sources, targets, held = refs[:count], refs[count : 2 * count], refs[2 * count : 3 * count]
    taken = [pltpu.make_async_copy(sources[i], held[i], sems.at[0, i]) for i in range(count)]
    given = [pltpu.make_async_copy(held[i], targets[i], sems.at[1, i]) for i in range(count)]
    for i in range(count):
        taken[i].start()
    for i in range(count):
        taken[i].wait()
        given[i].start()
    for i in range(count):
        given[i].wait()


def body(
    piece_tokens, decode_tokens, norm_gain, w_query, w_key, w_value, score_offset, context_length,
    prompt_keys, prompt_values, decode_keys, decode_values, decoding_cache_length, out_gain, w_out,
):
    n, tp = lax.axis_size("kv"), lax.axis_size("tp")
    nz, ny = grid_of(n)
    rows, model = piece_tokens.shape
    width = w_query.shape[1]
    seqs = decode_keys.shape[0]
    heads = width // HEAD
    assert nz % heads == 0 and tp % 2 == 0 and nz in (2, 4)
    parts = 2 if heads % 2 == 0 else 1
    share, band = heads // parts, width // parts
    cache_rows = prompt_keys.shape[0]
    vmem = pl.BlockSpec(memory_space=pltpu.VMEM)
    smem = pl.BlockSpec(memory_space=pltpu.SMEM)
    hbm = pl.BlockSpec(memory_space=pl.ANY)
    dma = pltpu.SemaphoreType.DMA

    def half(*shape):
        return pltpu.VMEM(shape, jnp.bfloat16)

    def full(*shape):
        return pltpu.VMEM(shape, jnp.float32)

    def result(*shape):
        return jax.ShapeDtypeStruct(shape, jnp.bfloat16)

    results = pl.pallas_call(
        functools.partial(attention_kernel, nz, ny, tp, heads, parts),
        out_shape=(
            result(rows, w_out.shape[1]), result(seqs, w_out.shape[1]), result(rows, width), result(rows, width),
            result(seqs, width), result(seqs, width),
        ),
        in_specs=[hbm] * 10 + [vmem] * 2 + [smem] * 3,
        out_specs=(vmem, vmem, hbm, hbm, vmem, vmem),
        scratch_shapes=[
            half(rows, model), half(seqs, model), half(model, width), half(model, width), half(model, width),
            half(*prompt_keys.shape), half(*prompt_values.shape), half(*decode_keys.shape), half(*decode_values.shape),
            half(*w_out.shape),
            half(rows + 16, model), half(parts, rows, band), half(rows, width), half(rows, width), half(16, width),
            half(rows + 16, tp * width),
            half(n, parts, rows, band), half(heads, cache_rows, HEAD), half(heads, HEAD, cache_rows),
            full(heads, cache_rows, 128), full(share, cache_rows, ny * rows),
            full(nz, parts, ny, band, rows), half(nz, parts, ny, band, rows), full(nz, parts, ny, 8, 128),
            half(nz, parts, ny, band, rows), full(nz, parts, ny, 8, 128), full(ny, band, rows), full(band, rows),
            half(nz, parts, band, rows), full(nz, parts, 8, 128), half(nz, parts, band, rows),
            full(nz, parts, 8, 128), full(parts, band, rows), full(parts, 8, 128),
            half(heads, 2 * rows, HEAD), half(n, 2 * rows, HEAD), half(heads * rows, HEAD),
            full(4, rows, heads * rows), full(4, HEAD, heads * rows), full(HEAD, heads * rows), full(8, heads * rows),
            half(heads, HEAD, rows), full(heads, 8, 128), half(heads, HEAD, rows), full(heads, 8, 128),
            half(parts, rows + 16, band), half(tp, parts, rows + 16, band),
            dma((ny, parts)), dma((nz, parts)), dma((nz, parts, ny)), dma((n, parts)),
            dma((nz,)), dma((ny,)), dma((nz, ny)), dma((n,)),
            dma((nz, parts, ny)), dma((nz, parts, ny)), dma((nz, parts, ny)), dma((nz, parts, ny)),
            dma((nz, parts)), dma((nz, parts)), dma((nz, parts)), dma((nz, parts)),
            dma((heads,)), dma((heads,)), dma((heads,)), dma((heads,)),
            dma((tp, parts)), dma((tp, parts)), dma((tp, parts)), dma((7,)), dma((3, 8)), dma((2,)),
            dma((parts,)),
        ],
        compiler_params=pltpu.CompilerParams(
            collective_id=0, has_side_effects=True, vmem_limit_bytes=60 * 1024 * 1024
        ),
        name="attend",
    )(
        piece_tokens, decode_tokens, w_query, w_key, w_value, prompt_keys, prompt_values, decode_keys, decode_values,
        w_out, norm_gain, out_gain, score_offset, context_length, decoding_cache_length,
    )
    kinds = [jax.ShapeDtypeStruct(r.shape, r.dtype) for r in results]
    return pl.pallas_call(
        deliver_kernel,
        out_shape=kinds,
        in_specs=[hbm] * len(kinds),
        out_specs=[hbm] * len(kinds),
        scratch_shapes=[pltpu.VMEM(k.shape, k.dtype) for k in kinds] + [dma((2, len(kinds)))],
        name="deliver",
    )(*results)


def solution(mesh):
    in_specs = (
        P("kv", None),
        P("kv", None),
        P(),
        P(None, "tp"),
        P(None, "tp"),
        P(None, "tp"),
        P(),
        P(),
        P("kv", "tp"),
        P("kv", "tp"),
        P("kv", None, "tp"),
        P("kv", None, "tp"),
        P("kv"),
        P(),
        P(None, "tp"),
    )
    out_specs = (
        P("kv", "tp"),
        P("kv", "tp"),
        P("kv", "tp"),
        P("kv", "tp"),
        P("kv", "tp"),
        P("kv", "tp"),
    )
    return jax.shard_map(body, mesh=mesh, in_specs=in_specs, out_specs=out_specs, check_vma=False)
```
